32 devices in a mesh: ra: 4 (over z), cb: 4 (over y, x), dp: 2 (over core).
Axes of the slice: x: 2, y: 2, z: 4, core: 2. Of those that a mesh axis runs over, the one named last changes fastest.
Arguments:
- tokens: bfloat16 [256, 2048], P('dp', 'ra'), may hold values from -200 to 200, as said below
- first_gain: float32 [2048], P('ra'), may hold values from 0.1 to 1.9
- first_gate: float32 [2048, 5632], P('ra', 'cb'), may hold values from -0.125 to 0.125
- first_gate_scale: float32 [5632], P('cb'), may hold values from 0.5 to 2
- first_up: float32 [2048, 5632], P('ra', 'cb'), may hold values from -0.125 to 0.125
- first_up_scale: float32 [5632], P('cb'), may hold values from 0.5 to 2
- first_down: float32 [5632, 2048], P('cb', 'ra'), may hold values from -0.078125 to 0.078125
- first_down_scale: float32 [2048], P('ra'), may hold values from 0.5 to 2
- second_gain: float32 [2048], P('ra'), may hold values from 0.1 to 1.9
- second_gate: float32 [2048, 5632], P('ra', 'cb'), may hold values from -0.125 to 0.125
- second_gate_scale: float32 [5632], P('cb'), may hold values from 0.5 to 2
- second_up: float32 [2048, 5632], P('ra', 'cb'), may hold values from -0.125 to 0.125
- second_up_scale: float32 [5632], P('cb'), may hold values from 0.5 to 2
- second_down: float32 [5632, 2048], P('cb', 'ra'), may hold values from -0.078125 to 0.078125
- second_down_scale: float32 [2048], P('ra'), may hold values from 0.5 to 2
Outputs:
- stream_out: bfloat16 [256, 2048], P('dp', 'ra')
The draws below stay inside these ranges and needn't reach their ends.
Inputs may be any that keep to these rules, and one draw needn't show every extreme that they name: `tokens`: Per-token and per-feature magnitudes vary.
All inputs are finite; a program needn't handle non-finite values.
Results may differ from the reference program's by a relative error of at most 0.039.
Values may be sent and summed in bfloat16 or wider, within the bound.
A program may use at most 64 MiB of HBM per device.

```python
import math
import jax
import jax.numpy as jnp
from jax import lax

D = 2048
FF = 5632
TOKENS = 256
N_CB = 4


def draw_tokens(key, part):
    key_base, key_rows = jax.random.split(jax.random.fold_in(key, 11), 2)
    position = jnp.arange(D, dtype=jnp.float32) / D
    base = jnp.clip(jax.random.normal(key_base, (TOKENS, D), jnp.float32), -6.0, 6.0)
    columns = 10.0 ** (0.5 * position)
    rows = jnp.exp(jax.random.uniform(key_rows, (TOKENS, 1), jnp.float32, 0.0, math.log(10.0)))
    values = jnp.clip(base * columns * rows / 4.0, -200.0, 200.0)
    return values.astype(jnp.bfloat16)


def level_of(own_key, dims, pieces, low, largest):
    level, own = 1.0, jax.random.fold_in(own_key, 6)
    for axis_at, shards_of in pieces:
        steps = jnp.exp(jax.random.uniform(jax.random.fold_in(own, axis_at), (shards_of,), jnp.float32, low / len(pieces), largest / len(pieces)))
        level = level * jnp.repeat(steps, dims[axis_at] // shards_of).reshape([-1 if axis == axis_at else 1 for axis in range(len(dims))])
    return level


def centred(own_key, extent, deviation, bound, pieces=(), kind=jnp.bfloat16):
    values = deviation * jax.random.normal(own_key, extent, jnp.float32)
    if pieces:
        values = values * level_of(own_key, extent, pieces, -0.22, 0.18)
    return jnp.clip(values, -bound, bound).astype(kind)


def setup_inputs(seed: int = 0) -> dict:
    keys = jax.random.split(jax.random.key(seed), 16)
    tokens = draw_tokens(jax.random.fold_in(keys[15], 71), 0)
    first_gain = jnp.clip(1.0 + 0.18 * jax.random.normal(keys[1], (D,), jnp.float32), 0.1, 1.9)
    first_gate = centred(keys[2], (D, FF), D ** -0.5, 0.125, ((0, 4), (1, 4)), jnp.float32)
    first_gate_scale = jnp.clip(jnp.exp(math.log(2.0) - 1.3862944 * jax.random.uniform(keys[3], (FF,), jnp.float32) ** level_of(keys[3], (FF,), ((0, 4),), -0.2, 0.2)), 0.5, 2.0)
    first_up = centred(keys[4], (D, FF), D ** -0.5, 0.125, ((0, 4), (1, 4)), jnp.float32)
    first_up_scale = jnp.clip(jnp.exp(math.log(2.0) - 1.3862944 * jax.random.uniform(keys[5], (FF,), jnp.float32) ** level_of(keys[5], (FF,), ((0, 4),), -0.2, 0.2)), 0.5, 2.0)
    first_down = centred(keys[6], (FF, D), FF ** -0.5, 0.078125, ((0, 4), (1, 4)), jnp.float32)
    first_down_scale = jnp.clip(jnp.exp(math.log(2.0) - 1.3862944 * jax.random.uniform(keys[7], (D,), jnp.float32) ** level_of(keys[7], (D,), ((0, 4),), -0.2, 0.2)), 0.5, 2.0)
    second_gain = jnp.clip(1.0 + 0.18 * jax.random.normal(keys[8], (D,), jnp.float32), 0.1, 1.9)
    second_gate = centred(keys[9], (D, FF), D ** -0.5, 0.125, ((0, 4), (1, 4)), jnp.float32)
    second_gate_scale = jnp.clip(jnp.exp(math.log(2.0) - 1.3862944 * jax.random.uniform(keys[10], (FF,), jnp.float32) ** level_of(keys[10], (FF,), ((0, 4),), -0.2, 0.2)), 0.5, 2.0)
    second_up = centred(keys[11], (D, FF), D ** -0.5, 0.125, ((0, 4), (1, 4)), jnp.float32)
    second_up_scale = jnp.clip(jnp.exp(math.log(2.0) - 1.3862944 * jax.random.uniform(keys[12], (FF,), jnp.float32) ** level_of(keys[12], (FF,), ((0, 4),), -0.2, 0.2)), 0.5, 2.0)
    second_down = centred(keys[13], (FF, D), FF ** -0.5, 0.078125, ((0, 4), (1, 4)), jnp.float32)
    second_down_scale = jnp.clip(jnp.exp(math.log(2.0) - 1.3862944 * jax.random.uniform(keys[14], (D,), jnp.float32) ** level_of(keys[14], (D,), ((0, 4),), -0.2, 0.2)), 0.5, 2.0)
    return {"tokens": tokens, "first_gain": first_gain, "first_gate": first_gate, "first_gate_scale": first_gate_scale, "first_up": first_up, "first_up_scale": first_up_scale, "first_down": first_down, "first_down_scale": first_down_scale, "second_gain": second_gain, "second_gate": second_gate, "second_gate_scale": second_gate_scale, "second_up": second_up, "second_up_scale": second_up_scale, "second_down": second_down, "second_down_scale": second_down_scale}


EPS = 1e-06
RESID = 0.5

def sublayer(stream, gain, w_gate, gate_scale, w_up, up_scale, w_down, down_scale):
    values = stream.astype(jnp.float32)
    mean_sq = lax.optimization_barrier(jnp.mean(values * values, -1, keepdims=True))
    normed = (values * lax.rsqrt(mean_sq + EPS) * gain).astype(jnp.bfloat16)
    gate = jnp.dot(normed, w_gate.astype(jnp.bfloat16), preferred_element_type=jnp.float32) * gate_scale
    up = jnp.dot(normed, w_up.astype(jnp.bfloat16), preferred_element_type=jnp.float32) * up_scale
    hidden = (jax.nn.silu(gate) * up).astype(jnp.bfloat16)
    down_b = w_down.astype(jnp.bfloat16)
    block = FF // N_CB
    branch = jnp.zeros((stream.shape[0], D), jnp.float32)
    for index in range(N_CB):
        partial_value = jnp.dot(hidden[:, index * block:(index + 1) * block], down_b[index * block:(index + 1) * block], preferred_element_type=jnp.float32)
        branch = branch + lax.optimization_barrier(partial_value.astype(jnp.bfloat16)).astype(jnp.float32)
    return (RESID * values + branch * down_scale).astype(jnp.bfloat16)

def reference(tokens, first_gain, first_gate, first_gate_scale, first_up, first_up_scale, first_down, first_down_scale, second_gain, second_gate, second_gate_scale, second_up, second_up_scale, second_down, second_down_scale):
    middle = sublayer(tokens, first_gain, first_gate, first_gate_scale, first_up, first_up_scale, first_down, first_down_scale)
    return sublayer(middle, second_gain, second_gate, second_gate_scale, second_up, second_up_scale, second_down, second_down_scale)
```

```python
import functools

import jax
import jax.numpy as jnp
from jax import lax
from jax.experimental import pallas as pl
from jax.experimental.pallas import tpu as pltpu
from jax.sharding import PartitionSpec as P

EPS = 1e-06
RESID = 0.5
MESH = pl.DeviceIdType.MESH
CHUNK = 128
LAG = 3
PIECES = 2


def kernel(
    n_ra, n_cb, width,
    tokens, gain1, gs1, us1, ds1, gain2, gs2, us2, ds2,
    wg1, wu1, wd1, wg2, wu2, wd2,
    out,
    wg, wu, wd, part, rs_send, rs_recv, hid, ss_send, ss_recv, inv, xs, stream, cb_send, cb_recv,
    wg_sem, wu_sem, wd_sem,
    rs_ss, rs_rs, ag_ss, ag_rs, sq_ss, sq_rs, cb_ss, cb_rs,
):
    p = lax.axis_index("ra")
    c = lax.axis_index("cb")
    tok = tokens.shape[0]
    half = tok // 2
    chunks = wg.shape[2] // CHUNK
    last = n_ra - 1
    phases = n_cb.bit_length() - 1
    rows_of = half // PIECES
    gates, ups, downs = (wg1, wg2), (wu1, wu2), (wd1, wd2)

    def cols(k):
        return pl.ds(pl.multiple_of(k * CHUNK, CHUNK), CHUNK)

    def load_pair(layer, k):
        return (
            pltpu.make_async_copy(gates[layer].at[:, cols(k)], wg.at[layer, :, cols(k)], wg_sem.at[layer, k]),
            pltpu.make_async_copy(ups[layer].at[:, cols(k)], wu.at[layer, :, cols(k)], wu_sem.at[layer, k]),
        )

    def load_down(layer):
        return pltpu.make_async_copy(downs[layer], wd.at[layer], wd_sem.at[layer])

    def start_pairs(layer):
        @pl.loop(0, chunks)
        def _(k):
            for copy in load_pair(layer, k):
                copy.start()

    start_pairs(0)
    load_down(0).start()

    def partner(bit):
        return c + bit - 2 * bit * ((c // bit) % 2)

    barrier = pltpu.get_barrier_semaphore()

    @pl.when(p > 0)
    def _():
        pl.semaphore_signal(barrier, inc=1, device_id={"ra": p - 1}, device_id_type=MESH)

    @pl.when(p < last)
    def _():
        pl.semaphore_signal(barrier, inc=1, device_id={"ra": p + 1}, device_id_type=MESH)

    for b in range(phases):
        pl.semaphore_signal(barrier, inc=1, device_id={"cb": partner(1 << b)}, device_id_type=MESH)

    def place(way):
        return (p, p + 1, p - 1) if way == 0 else (last - p, p - 1, p + 1)

    def rs_copy(layer, way, k, to):
        return pltpu.make_async_remote_copy(
            src_ref=rs_send.at[layer, way, k], dst_ref=rs_recv.at[layer, way, k],
            send_sem=rs_ss.at[layer, way, k], recv_sem=rs_rs.at[layer, way, k],
            device_id={"ra": to}, device_id_type=MESH)

    def sq_copy(layer, way, to):
        return pltpu.make_async_remote_copy(
            src_ref=ss_send.at[layer, way], dst_ref=ss_recv.at[layer, way],
            send_sem=sq_ss.at[layer, way], recv_sem=sq_rs.at[layer, way],
            device_id={"ra": to}, device_id_type=MESH)

    def ag_copy(layer, way, k, to):
        piece = hid.at[layer, pl.ds(way * half, half), cols(k)]
        return pltpu.make_async_remote_copy(
            src_ref=piece, dst_ref=piece,
            send_sem=ag_ss.at[layer, way, k], recv_sem=ag_rs.at[layer, way, k],
            device_id={"ra": to}, device_id_type=MESH)

    def cb_copy(layer, phase, h, g):
        bit = 1 << ((phase + h) % phases)
        return pltpu.make_async_remote_copy(
            src_ref=cb_send.at[layer, phase, h, g], dst_ref=cb_recv.at[layer, phase, h, g],
            send_sem=cb_ss.at[layer, phase, h, g], recv_sem=cb_rs.at[layer, phase, h, g],
            device_id={"cb": partner(bit)}, device_id_type=MESH)

    for layer in range(2):
        gain = (gain1, gain2)[layer]
        gscale, uscale, dscale = (gs1, gs2)[layer], (us1, us2)[layer], (ds1, ds2)[layer]
        values = (tokens if layer == 0 else stream)[...].astype(jnp.float32)
        xs[...] = (values * gain[...]).astype(jnp.bfloat16)
        sums = jnp.sum(values * values, axis=-1, keepdims=True)
        flat = jnp.broadcast_to(sums, (tok, 128)).T[:8]
        ss_send[layer, 0] = flat
        ss_send[layer, 1] = flat
        if layer == 0:
            pl.semaphore_wait(barrier, (p > 0).astype(jnp.int32) + (p < last).astype(jnp.int32) + phases)
        for way in range(2):
            at, ahead, _ = place(way)

            @pl.when(at == 0)
            def _():
                sq_copy(layer, way, ahead).start()

        @pl.loop(0, chunks + LAG * 2 * last)
        def _(t):
            @pl.when(t < chunks)
            def _():
                for copy in load_pair(layer, t):
                    copy.wait()
                w = jnp.concatenate(
                    [wg[layer, :, cols(t)].astype(jnp.bfloat16), wu[layer, :, cols(t)].astype(jnp.bfloat16)], axis=1)
                prod = jnp.dot(xs[...], w, preferred_element_type=jnp.float32)
                part[t] = prod
                for way in range(2):
                    at, ahead, _ = place(way)

                    @pl.when(at == 0)
                    def _():
                        rs_send[layer, way, t] = prod[way * half:(way + 1) * half].astype(jnp.bfloat16)
                        rs_copy(layer, way, t, ahead).start()

            for way in range(2):
                at, ahead, behind = place(way)
                lo = way * half
                k = t - LAG * at
                inside = (k >= 0) & (k < chunks) & (at > 0)

                @pl.when(inside & (k == 0))
                def _():
                    sq_copy(layer, way, ahead).wait_recv()
                    total = ss_recv[layer, way] + ss_send[layer, way]

                    @pl.when(at < last)
                    def _():
                        ss_send[layer, way] = total
                        sq_copy(layer, way, ahead).start()

                    @pl.when(at == last)
                    def _():
                        column = jnp.broadcast_to(total[:1], (128, tok)).T
                        inv[way] = lax.rsqrt(column[lo:lo + half] / width + EPS)

                @pl.when(inside)
                def _():
                    rs_copy(layer, way, k, ahead).wait_recv()
                    total = rs_recv[layer, way, k].astype(jnp.float32) + part[k, lo:lo + half, :]

                    @pl.when(at < last)
                    def _():
                        rs_send[layer, way, k] = total.astype(jnp.bfloat16)
                        rs_copy(layer, way, k, ahead).start()

                    @pl.when(at == last)
                    def _():
                        scale = inv[way]
                        gate = total[:, :CHUNK] * scale * gscale[:, cols(k)]
                        up = total[:, CHUNK:] * scale * uscale[:, cols(k)]
                        hidden = gate / (1.0 + jnp.exp(-gate)) * up
                        hid[layer, lo:lo + half, cols(k)] = hidden.astype(jnp.bfloat16)
                        ag_copy(layer, way, k, behind).start()

                j = t - LAG * (2 * last - at)

                @pl.when((j >= 0) & (j < chunks) & (at < last))
                def _():
                    ag_copy(layer, way, j, behind).wait_recv()

                    @pl.when(at > 0)
                    def _():
                        ag_copy(layer, way, j, behind).start()

            if layer == 0:
                @pl.when(t == chunks)
                def _():
                    start_pairs(1)
                    load_down(1).start()

        load_down(layer).wait()
        down = jnp.dot(hid[layer], wd[layer].astype(jnp.bfloat16), preferred_element_type=jnp.float32)
        order = [(h, g) for g in range(PIECES) for h in range(2)]
        for h, g in order:
            lo = h * half + g * rows_of
            cb_send[layer, 0, h, g] = down[lo:lo + rows_of].astype(jnp.bfloat16)
            cb_copy(layer, 0, h, g).start()
        for phase in range(phases):
            for h, g in order:
                cb_copy(layer, phase, h, g).wait_recv()
                total = cb_send[layer, phase, h, g].astype(jnp.float32) + cb_recv[layer, phase, h, g].astype(jnp.float32)
                if phase < phases - 1:
                    cb_send[layer, phase + 1, h, g] = total.astype(jnp.bfloat16)
                    cb_copy(layer, phase + 1, h, g).start()
                else:
                    lo = h * half + g * rows_of
                    old = (tokens if layer == 0 else stream)[lo:lo + rows_of, :].astype(jnp.float32)
                    new = (RESID * old + total * dscale[...]).astype(jnp.bfloat16)
                    if layer == 0:
                        stream[lo:lo + rows_of, :] = new
                    else:
                        out[lo:lo + rows_of, :] = new

    for layer in range(2):
        for way in range(2):
            at, ahead, behind = place(way)

            @pl.when(at < last)
            def _():
                sq_copy(layer, way, ahead).wait_send()

                @pl.loop(0, chunks)
                def _(k):
                    rs_copy(layer, way, k, ahead).wait_send()

            @pl.when(at > 0)
            def _():
                @pl.loop(0, chunks)
                def _(k):
                    ag_copy(layer, way, k, behind).wait_send()

        for phase in range(phases):
            for h in range(2):
                for g in range(PIECES):
                    cb_copy(layer, phase, h, g).wait_send()


def solution(mesh):
    n_ra, n_cb = mesh.shape["ra"], mesh.shape["cb"]
    names = ("tokens", "g1", "wg1", "gs1", "wu1", "us1", "wd1", "ds1", "g2", "wg2", "gs2", "wu2", "us2", "wd2", "ds2")

    def body(*args):
        a = dict(zip(names, args))
        small = [a[k].reshape(1, -1) for k in ("g1", "gs1", "us1", "ds1", "g2", "gs2", "us2", "ds2")]
        big = [a[k] for k in ("wg1", "wu1", "wd1", "wg2", "wu2", "wd2")]
        tok, dim = a["tokens"].shape
        ff = a["wg1"].shape[1]
        chunks, half, phases = ff // CHUNK, tok // 2, n_cb.bit_length() - 1
        f32, bf16, dma = jnp.float32, jnp.bfloat16, pltpu.SemaphoreType.DMA
        vmem = pl.BlockSpec(memory_space=pltpu.VMEM)
        piece = (2, phases, 2, PIECES)
        return pl.pallas_call(
            functools.partial(kernel, n_ra, n_cb, dim * n_ra),
            out_shape=jax.ShapeDtypeStruct((tok, dim), bf16),
            in_specs=[vmem] * 9 + [pl.BlockSpec(memory_space=pl.ANY)] * 6,
            out_specs=vmem,
            scratch_shapes=[
                pltpu.VMEM((2, dim, ff), f32), pltpu.VMEM((2, dim, ff), f32), pltpu.VMEM((2, ff, dim), f32),
                pltpu.VMEM((chunks, tok, 2 * CHUNK), f32),
                pltpu.VMEM((2, 2, chunks, half, 2 * CHUNK), bf16),
                pltpu.VMEM((2, 2, chunks, half, 2 * CHUNK), bf16),
                pltpu.VMEM((2, tok, ff), bf16),
                pltpu.VMEM((2, 2, 8, tok), f32), pltpu.VMEM((2, 2, 8, tok), f32),
                pltpu.VMEM((2, half, 128), f32),
                pltpu.VMEM((tok, dim), bf16), pltpu.VMEM((tok, dim), bf16),
                pltpu.VMEM(piece + (half // PIECES, dim), bf16), pltpu.VMEM(piece + (half // PIECES, dim), bf16),
                dma((2, chunks)), dma((2, chunks)), dma((2,)),
                dma((2, 2, chunks)), dma((2, 2, chunks)), dma((2, 2, chunks)), dma((2, 2, chunks)),
                dma((2, 2)), dma((2, 2)), dma(piece), dma(piece),
            ],
            compiler_params=pltpu.CompilerParams(
                collective_id=0, has_side_effects=True, vmem_limit_bytes=56 * 1024 * 1024),
        )(a["tokens"], *small, *big)

    in_specs = (
        P("dp", "ra"),
        P("ra"), P("ra", "cb"), P("cb"), P("ra", "cb"), P("cb"), P("cb", "ra"), P("ra"),
        P("ra"), P("ra", "cb"), P("cb"), P("ra", "cb"), P("cb"), P("cb", "ra"), P("ra"),
    )
    return jax.shard_map(body, mesh=mesh, in_specs=in_specs, out_specs=P("dp", "ra"), check_vma=False)
```

```python
import functools

import jax
import jax.numpy as jnp
from jax import lax
from jax.experimental import pallas as pl
from jax.experimental.pallas import tpu as pltpu
from jax.sharding import PartitionSpec as P

EPS = 1e-06
RESID = 0.5
MESH = pl.DeviceIdType.MESH
CHUNK = 128
LAG = 5
PIECES = 2


def kernel(
    n_ra, n_cb, width,
    tokens_in, gain1_in, gs1_in, us1_in, ds1_in, gain2_in, gs2_in, us2_in, ds2_in,
    wg1, wu1, wd1, wg2, wu2, wd2,
    out,
    tokens, gain1, gs1, us1, ds1, gain2, gs2, us2, ds2,
    wg, wu, wd, part, rs_send, rs_recv, hid, ss_send, ss_recv, inv, xs, stream, cb_send, cb_recv,
    in_sem, wg_sem, wu_sem, wd_sem,
    rs_ss, rs_rs, ag_ss, ag_rs, sq_ss, sq_rs, cb_ss, cb_rs,
):
    p = lax.axis_index("ra")
    c = lax.axis_index("cb")
    tok = tokens.shape[0]
    half = tok // 2
    chunks = wg.shape[2] // CHUNK
    last = n_ra - 1
    phases = n_cb.bit_length() - 1
    rows_of = half // PIECES
    gates, ups, downs = (wg1, wg2), (wu1, wu2), (wd1, wd2)

    def cols(k):
        return pl.ds(pl.multiple_of(k * CHUNK, CHUNK), CHUNK)

    def load_pair(layer, k):
        return (
            pltpu.make_async_copy(gates[layer].at[:, cols(k)], wg.at[layer, :, cols(k)], wg_sem.at[layer, k]),
            pltpu.make_async_copy(ups[layer].at[:, cols(k)], wu.at[layer, :, cols(k)], wu_sem.at[layer, k]),
        )

    def load_down(layer):
        return pltpu.make_async_copy(downs[layer], wd.at[layer], wd_sem.at[layer])

    def start_pairs(layer):
        @pl.loop(0, chunks)
        def _(k):
            for copy in load_pair(layer, k):
                copy.start()

    small = [
        pltpu.make_async_copy(a, b, in_sem.at[i])
        for i, (a, b) in enumerate((
            (tokens_in, tokens), (gain1_in, gain1), (gs1_in, gs1), (us1_in, us1), (ds1_in, ds1),
            (gain2_in, gain2), (gs2_in, gs2), (us2_in, us2), (ds2_in, ds2)))
    ]
    for copy in small:
        copy.start()
    start_pairs(0)
    load_down(0).start()

    def partner(bit):
        return c + bit - 2 * bit * ((c // bit) % 2)

    barrier = pltpu.get_barrier_semaphore()

    @pl.when(p > 0)
    def _():
        pl.semaphore_signal(barrier, inc=1, device_id={"ra": p - 1}, device_id_type=MESH)

    @pl.when(p < last)
    def _():
        pl.semaphore_signal(barrier, inc=1, device_id={"ra": p + 1}, device_id_type=MESH)

    for b in range(phases):
        pl.semaphore_signal(barrier, inc=1, device_id={"cb": partner(1 << b)}, device_id_type=MESH)

    mid = n_ra // 2
    delay = chunks
    final = max(LAG * mid, delay + LAG * (last - mid)) if last > mid else LAG * mid
    sides = range(2 if last > mid else 1)

    def place(way):
        return (p, p + 1, p - 1) if way == 0 else (last - p, p - 1, p + 1)

    def role(way):
        at, ahead, behind = place(way)
        side = (at > mid).astype(jnp.int32)
        hops = at + side * (last - 2 * at)
        inward = ahead + side * (behind - ahead)
        return at, side, hops, inward, ahead + behind - inward

    def rs_copy(layer, way, side, k, to):
        return pltpu.make_async_remote_copy(
            src_ref=rs_send.at[layer, way, k], dst_ref=rs_recv.at[layer, way, side, k],
            send_sem=rs_ss.at[layer, way, k], recv_sem=rs_rs.at[layer, way, side, k],
            device_id={"ra": to}, device_id_type=MESH)

    def sq_copy(layer, way, side, to):
        return pltpu.make_async_remote_copy(
            src_ref=ss_send.at[layer, way], dst_ref=ss_recv.at[layer, way, side],
            send_sem=sq_ss.at[layer, way], recv_sem=sq_rs.at[layer, way, side],
            device_id={"ra": to}, device_id_type=MESH)

    def ag_copy(layer, way, side, k, to):
        piece = hid.at[layer, pl.ds(way * half, half), cols(k)]
        return pltpu.make_async_remote_copy(
            src_ref=piece, dst_ref=piece,
            send_sem=ag_ss.at[layer, way, side, k], recv_sem=ag_rs.at[layer, way, k],
            device_id={"ra": to}, device_id_type=MESH)

    def cb_copy(layer, phase, h, g):
        bit = 1 << ((phase + h) % phases)
        return pltpu.make_async_remote_copy(
            src_ref=cb_send.at[layer, phase, h, g], dst_ref=cb_recv.at[layer, phase, h, g],
            send_sem=cb_ss.at[layer, phase, h, g], recv_sem=cb_rs.at[layer, phase, h, g],
            device_id={"cb": partner(bit)}, device_id_type=MESH)

    for copy in small:
        copy.wait()
    for layer in range(2):
        gain = (gain1, gain2)[layer]
        gscale, uscale, dscale = (gs1, gs2)[layer], (us1, us2)[layer], (ds1, ds2)[layer]
        values = (tokens if layer == 0 else stream)[...].astype(jnp.float32)
        xs[...] = (values * gain[...][None, :]).astype(jnp.bfloat16)
        sums = jnp.sum(values * values, axis=-1, keepdims=True)
        flat = jnp.broadcast_to(sums, (tok, 128)).T[:8]
        ss_send[layer, 0] = flat
        ss_send[layer, 1] = flat
        if layer == 0:
            pl.semaphore_wait(barrier, (p > 0).astype(jnp.int32) + (p < last).astype(jnp.int32) + phases)
        for way in range(2):
            at, side, hops, inward, _ = role(way)

            @pl.when((hops == 0) & (at != mid))
            def _():
                sq_copy(layer, way, side, inward).start()

        @pl.loop(0, chunks + final + LAG * mid)
        def _(t):
            @pl.when(t < chunks)
            def _():
                for copy in load_pair(layer, t):
                    copy.wait()
                w = jnp.concatenate(
                    [wg[layer, :, cols(t)].astype(jnp.bfloat16), wu[layer, :, cols(t)].astype(jnp.bfloat16)], axis=1)
                part[t] = jnp.dot(xs[...], w, preferred_element_type=jnp.float32)

            for way in range(2):
                at, side, hops, inward, outward = role(way)
                lo = way * half
                k = t - delay * side - LAG * hops
                inside = (k >= 0) & (k < chunks) & (at != mid)

                @pl.when(inside & (hops == 0))
                def _():
                    rs_send[layer, way, k] = part[k, lo:lo + half, :].astype(jnp.bfloat16)
                    rs_copy(layer, way, side, k, inward).start()

                @pl.when(inside & (hops > 0))
                def _():
                    @pl.when(k == 0)
                    def _():
                        sq_copy(layer, way, side, inward).wait_recv()
                        ss_send[layer, way] = ss_recv[layer, way, side] + ss_send[layer, way]
                        sq_copy(layer, way, side, inward).start()

                    rs_copy(layer, way, side, k, inward).wait_recv()
                    total = rs_recv[layer, way, side, k].astype(jnp.float32) + part[k, lo:lo + half, :]
                    rs_send[layer, way, k] = total.astype(jnp.bfloat16)
                    rs_copy(layer, way, side, k, inward).start()

                m = t - final

                @pl.when((m >= 0) & (m < chunks) & (at == mid))
                def _():
                    @pl.when(m == 0)
                    def _():
                        total = ss_send[layer, way]
                        for s in sides:
                            sq_copy(layer, way, s, inward).wait_recv()
                            total += ss_recv[layer, way, s]
                        column = jnp.broadcast_to(total[:1], (128, tok)).T
                        inv[way] = lax.rsqrt(column[lo:lo + half] / width + EPS)

                    total = part[m, lo:lo + half, :]
                    for s in sides:
                        rs_copy(layer, way, s, m, inward).wait_recv()
                        total += rs_recv[layer, way, s, m].astype(jnp.float32)
                    scale = inv[way]
                    gate = total[:, :CHUNK] * scale * gscale[cols(m)][None, :]
                    up = total[:, CHUNK:] * scale * uscale[cols(m)][None, :]
                    hidden = gate / (1.0 + jnp.exp(-gate)) * up
                    hid[layer, lo:lo + half, cols(m)] = hidden.astype(jnp.bfloat16)
                    for s in sides:
                        ag_copy(layer, way, s, m, place(way)[2 - s]).start()

                j = t - final - LAG * (at - mid) * (2 * side - 1)

                @pl.when((j >= 0) & (j < chunks) & (at != mid))
                def _():
                    ag_copy(layer, way, side, j, outward).wait_recv()

                    @pl.when(hops > 0)
                    def _():
                        ag_copy(layer, way, side, j, outward).start()

            if layer == 0:
                @pl.when(t == chunks)
                def _():
                    start_pairs(1)
                    load_down(1).start()

        load_down(layer).wait()
        down = jnp.dot(hid[layer], wd[layer].astype(jnp.bfloat16), preferred_element_type=jnp.float32)
        order = [(h, g) for g in range(PIECES) for h in range(2)]
        for h, g in order:
            lo = h * half + g * rows_of
            cb_send[layer, 0, h, g] = down[lo:lo + rows_of].astype(jnp.bfloat16)
            cb_copy(layer, 0, h, g).start()
        for phase in range(phases):
            for h, g in order:
                cb_copy(layer, phase, h, g).wait_recv()
                total = cb_send[layer, phase, h, g].astype(jnp.float32) + cb_recv[layer, phase, h, g].astype(jnp.float32)
                if phase < phases - 1:
                    cb_send[layer, phase + 1, h, g] = total.astype(jnp.bfloat16)
                    cb_copy(layer, phase + 1, h, g).start()
                else:
                    lo = h * half + g * rows_of
                    old = (tokens if layer == 0 else stream)[lo:lo + rows_of, :].astype(jnp.float32)
                    new = (RESID * old + total * dscale[...][None, :]).astype(jnp.bfloat16)
                    if layer == 0:
                        stream[lo:lo + rows_of, :] = new
                    else:
                        out[lo:lo + rows_of, :] = new

    for layer in range(2):
        for way in range(2):
            at, side, hops, inward, outward = role(way)

            @pl.when(at != mid)
            def _():
                sq_copy(layer, way, side, inward).wait_send()

                @pl.loop(0, chunks)
                def _(k):
                    rs_copy(layer, way, side, k, inward).wait_send()

            @pl.when((at != mid) & (hops > 0))
            def _():
                @pl.loop(0, chunks)
                def _(k):
                    ag_copy(layer, way, side, k, outward).wait_send()

            @pl.when(at == mid)
            def _():
                @pl.loop(0, chunks)
                def _(k):
                    for s in sides:
                        ag_copy(layer, way, s, k, outward).wait_send()

        for phase in range(phases):
            for h in range(2):
                for g in range(PIECES):
                    cb_copy(layer, phase, h, g).wait_send()


def solution(mesh):
    n_ra, n_cb = mesh.shape["ra"], mesh.shape["cb"]
    names = ("tokens", "g1", "wg1", "gs1", "wu1", "us1", "wd1", "ds1", "g2", "wg2", "gs2", "wu2", "us2", "wd2", "ds2")

    def body(*args):
        a = dict(zip(names, args))
        small = [a[k] for k in ("g1", "gs1", "us1", "ds1", "g2", "gs2", "us2", "ds2")]
        big = [a[k] for k in ("wg1", "wu1", "wd1", "wg2", "wu2", "wd2")]
        tok, dim = a["tokens"].shape
        ff = a["wg1"].shape[1]
        chunks, half, phases = ff // CHUNK, tok // 2, n_cb.bit_length() - 1
        f32, bf16, dma = jnp.float32, jnp.bfloat16, pltpu.SemaphoreType.DMA
        vmem = pl.BlockSpec(memory_space=pltpu.VMEM)
        piece = (2, phases, 2, PIECES)
        return pl.pallas_call(
            functools.partial(kernel, n_ra, n_cb, dim * n_ra),
            out_shape=jax.ShapeDtypeStruct((tok, dim), bf16),
            in_specs=[pl.BlockSpec(memory_space=pl.ANY)] * 15,
            out_specs=vmem,
            scratch_shapes=[
                pltpu.VMEM((tok, dim), bf16), *[pltpu.VMEM(v.shape, f32) for v in small],
                pltpu.VMEM((2, dim, ff), f32), pltpu.VMEM((2, dim, ff), f32), pltpu.VMEM((2, ff, dim), f32),
                pltpu.VMEM((chunks, tok, 2 * CHUNK), f32),
                pltpu.VMEM((2, 2, chunks, half, 2 * CHUNK), bf16),
                pltpu.VMEM((2, 2, 2, chunks, half, 2 * CHUNK), bf16),
                pltpu.VMEM((2, tok, ff), bf16),
                pltpu.VMEM((2, 2, 8, tok), f32), pltpu.VMEM((2, 2, 2, 8, tok), f32),
                pltpu.VMEM((2, half, 128), f32),
                pltpu.VMEM((tok, dim), bf16), pltpu.VMEM((tok, dim), bf16),
                pltpu.VMEM(piece + (half // PIECES, dim), bf16), pltpu.VMEM(piece + (half // PIECES, dim), bf16),
                dma((9,)), dma((2, chunks)), dma((2, chunks)), dma((2,)),
                dma((2, 2, chunks)), dma((2, 2, 2, chunks)), dma((2, 2, 2, chunks)), dma((2, 2, chunks)),
                dma((2, 2)), dma((2, 2, 2)), dma(piece), dma(piece),
            ],
            compiler_params=pltpu.CompilerParams(
                collective_id=0, has_side_effects=True, vmem_limit_bytes=56 * 1024 * 1024),
        )(a["tokens"], *small, *big)

    in_specs = (
        P("dp", "ra"),
        P("ra"), P("ra", "cb"), P("cb"), P("ra", "cb"), P("cb"), P("cb", "ra"), P("ra"),
        P("ra"), P("ra", "cb"), P("cb"), P("ra", "cb"), P("cb"), P("cb", "ra"), P("ra"),
    )
    return jax.shard_map(body, mesh=mesh, in_specs=in_specs, out_specs=P("dp", "ra"), check_vma=False)
```

```python
import functools
import itertools

import jax
import jax.numpy as jnp
from jax import lax
from jax.experimental import pallas as pl
from jax.experimental.pallas import tpu as pltpu
from jax.sharding import PartitionSpec as P

EPS = 1e-06
RESID = 0.5
MESH = pl.DeviceIdType.MESH
CHUNK = 128
LAG = 5
FAR = 4
PIECES = 2


def kernel(
    n_ra, n_cb, width,
    tokens_in, gain1_in, gs1_in, us1_in, ds1_in, gain2_in, gs2_in, us2_in, ds2_in,
    wg1, wu1, wd1, wg2, wu2, wd2,
    out,
    tokens, gain1, gs1, us1, ds1, gain2, gs2, us2, ds2,
    wg, wu, wd, part, rs_send, rs_recv, hid, ss_send, ss_recv, inv, xs, stream, cb_send, cb_recv,
    in_sem, wg_sem, wu_sem, wd_sem,
    rs_ss, rs_rs, ag_ss, ag_rs, sq_ss, sq_rs, cb_ss, cb_rs,
):
    p = lax.axis_index("ra")
    c = lax.axis_index("cb")
    tok = tokens.shape[0]
    half = tok // 2
    chunks = wg.shape[2] // CHUNK
    last = n_ra - 1
    phases = n_cb.bit_length() - 1
    rows_of = half // PIECES
    gates, ups, downs = (wg1, wg2), (wu1, wu2), (wd1, wd2)

    def cols(k):
        return pl.ds(pl.multiple_of(k * CHUNK, CHUNK), CHUNK)

    def load_pair(layer, k):
        return (
            pltpu.make_async_copy(gates[layer].at[:, cols(k)], wg.at[layer, :, cols(k)], wg_sem.at[layer, k]),
            pltpu.make_async_copy(ups[layer].at[:, cols(k)], wu.at[layer, :, cols(k)], wu_sem.at[layer, k]),
        )

    def load_down(layer):
        return pltpu.make_async_copy(downs[layer], wd.at[layer], wd_sem.at[layer])

    def start_pairs(layer):
        @pl.loop(0, chunks)
        def _(k):
            for copy in load_pair(layer, k):
                copy.start()

    small = [
        pltpu.make_async_copy(a, b, in_sem.at[i])
        for i, (a, b) in enumerate((
            (tokens_in, tokens), (gain1_in, gain1), (gs1_in, gs1), (us1_in, us1), (ds1_in, ds1),
            (gain2_in, gain2), (gs2_in, gs2), (us2_in, us2), (ds2_in, ds2)))
    ]
    for copy in small:
        copy.start()
    start_pairs(0)
    load_down(0).start()

    def partner(bit):
        return c + bit - 2 * bit * ((c // bit) % 2)

    barrier = pltpu.get_barrier_semaphore()

    @pl.when(p > 0)
    def _():
        pl.semaphore_signal(barrier, inc=1, device_id={"ra": p - 1}, device_id_type=MESH)

    @pl.when(p < last)
    def _():
        pl.semaphore_signal(barrier, inc=1, device_id={"ra": p + 1}, device_id_type=MESH)

    for b in range(phases):
        pl.semaphore_signal(barrier, inc=1, device_id={"cb": partner(1 << b)}, device_id_type=MESH)

    mid = n_ra // 2
    both = range(2 if last > mid else 1)
    near_delay = chunks - FAR
    groups = (
        (last, 0, FAR, range(1), 0, LAG * last),
        (mid, FAR, chunks, both, near_delay, max(LAG * mid, near_delay + LAG * (last - mid))),
    )
    ticks = max(end + final + LAG * owner for owner, _, end, _, _, final in groups)

    def place(way):
        return (p, p + 1, p - 1) if way == 0 else (last - p, p - 1, p + 1)

    def role(way, owner):
        at, ahead, behind = place(way)
        side = (at > owner).astype(jnp.int32)
        hops = at + side * (last - 2 * at)
        inward = ahead + side * (behind - ahead)
        return at, side, hops, inward, ahead + behind - inward

    def rs_copy(layer, way, side, k, to):
        return pltpu.make_async_remote_copy(
            src_ref=rs_send.at[layer, way, k], dst_ref=rs_recv.at[layer, way, side, k],
            send_sem=rs_ss.at[layer, way, k], recv_sem=rs_rs.at[layer, way, side, k],
            device_id={"ra": to}, device_id_type=MESH)

    def sq_copy(layer, way, group, side, to):
        return pltpu.make_async_remote_copy(
            src_ref=ss_send.at[layer, way, group], dst_ref=ss_recv.at[layer, way, group, side],
            send_sem=sq_ss.at[layer, way, group], recv_sem=sq_rs.at[layer, way, group, side],
            device_id={"ra": to}, device_id_type=MESH)

    def ag_copy(layer, way, side, k, to):
        piece = hid.at[layer, pl.ds(way * half, half), cols(k)]
        return pltpu.make_async_remote_copy(
            src_ref=piece, dst_ref=piece,
            send_sem=ag_ss.at[layer, way, side, k], recv_sem=ag_rs.at[layer, way, k],
            device_id={"ra": to}, device_id_type=MESH)

    def cb_copy(layer, phase, h, g):
        bit = 1 << ((phase + h) % phases)
        return pltpu.make_async_remote_copy(
            src_ref=cb_send.at[layer, phase, h, g], dst_ref=cb_recv.at[layer, phase, h, g],
            send_sem=cb_ss.at[layer, phase, h, g], recv_sem=cb_rs.at[layer, phase, h, g],
            device_id={"cb": partner(bit)}, device_id_type=MESH)

    for copy in small:
        copy.wait()
    for layer in range(2):
        gain = (gain1, gain2)[layer]
        gscale, uscale, dscale = (gs1, gs2)[layer], (us1, us2)[layer], (ds1, ds2)[layer]
        values = (tokens if layer == 0 else stream)[...].astype(jnp.float32)
        xs[...] = (values * gain[...][None, :]).astype(jnp.bfloat16)
        sums = jnp.sum(values * values, axis=-1, keepdims=True)
        flat = jnp.broadcast_to(sums, (tok, 128)).T[:8]
        for way in range(2):
            for group in range(2):
                ss_send[layer, way, group] = flat
        if layer == 0:
            pl.semaphore_wait(barrier, (p > 0).astype(jnp.int32) + (p < last).astype(jnp.int32) + phases)
        for way in range(2):
            for group, (owner, *_) in enumerate(groups):
                at, side, hops, inward, _ = role(way, owner)

                @pl.when((hops == 0) & (at != owner))
                def _():
                    sq_copy(layer, way, group, side, inward).start()

        @pl.loop(0, ticks)
        def _(t):
            @pl.when(t < chunks)
            def _():
                for copy in load_pair(layer, t):
                    copy.wait()
                w = jnp.concatenate(
                    [wg[layer, :, cols(t)].astype(jnp.bfloat16), wu[layer, :, cols(t)].astype(jnp.bfloat16)], axis=1)
                part[t] = jnp.dot(xs[...], w, preferred_element_type=jnp.float32)

            for way, (group, (owner, first, end, sides, delay, final)) in itertools.product(range(2), enumerate(groups)):
                at, side, hops, inward, outward = role(way, owner)
                lo = way * half
                k = t - delay * side - LAG * hops
                inside = (k >= first) & (k < end) & (at != owner)

                @pl.when(inside & (hops == 0))
                def _():
                    rs_send[layer, way, k] = part[k, lo:lo + half, :].astype(jnp.bfloat16)
                    rs_copy(layer, way, side, k, inward).start()

                @pl.when(inside & (hops > 0))
                def _():
                    @pl.when(k == first)
                    def _():
                        sq_copy(layer, way, group, side, inward).wait_recv()
                        ss_send[layer, way, group] = ss_recv[layer, way, group, side] + ss_send[layer, way, group]
                        sq_copy(layer, way, group, side, inward).start()

                    rs_copy(layer, way, side, k, inward).wait_recv()
                    total = rs_recv[layer, way, side, k].astype(jnp.float32) + part[k, lo:lo + half, :]
                    rs_send[layer, way, k] = total.astype(jnp.bfloat16)
                    rs_copy(layer, way, side, k, inward).start()

                m = t - final

                @pl.when((m >= first) & (m < end) & (at == owner))
                def _():
                    @pl.when(m == first)
                    def _():
                        total = ss_send[layer, way, group]
                        for s in sides:
                            sq_copy(layer, way, group, s, inward).wait_recv()
                            total += ss_recv[layer, way, group, s]
                        column = jnp.broadcast_to(total[:1], (128, tok)).T
                        inv[way] = lax.rsqrt(column[lo:lo + half] / width + EPS)

                    total = part[m, lo:lo + half, :]
                    for s in sides:
                        rs_copy(layer, way, s, m, inward).wait_recv()
                        total += rs_recv[layer, way, s, m].astype(jnp.float32)
                    scale = inv[way]
                    gate = total[:, :CHUNK] * scale * gscale[cols(m)][None, :]
                    up = total[:, CHUNK:] * scale * uscale[cols(m)][None, :]
                    hidden = gate / (1.0 + jnp.exp(-gate)) * up
                    hid[layer, lo:lo + half, cols(m)] = hidden.astype(jnp.bfloat16)
                    for s in sides:
                        ag_copy(layer, way, s, m, place(way)[2 - s]).start()

                j = t - final - LAG * (at - owner) * (2 * side - 1)

                @pl.when((j >= first) & (j < end) & (at != owner))
                def _():
                    ag_copy(layer, way, side, j, outward).wait_recv()

                    @pl.when(hops > 0)
                    def _():
                        ag_copy(layer, way, side, j, outward).start()

            if layer == 0:
                @pl.when(t == chunks)
                def _():
                    start_pairs(1)
                    load_down(1).start()

        load_down(layer).wait()
        down = jnp.dot(hid[layer], wd[layer].astype(jnp.bfloat16), preferred_element_type=jnp.float32)
        order = [(h, g) for g in range(PIECES) for h in range(2)]
        for h, g in order:
            lo = h * half + g * rows_of
            cb_send[layer, 0, h, g] = down[lo:lo + rows_of].astype(jnp.bfloat16)
            cb_copy(layer, 0, h, g).start()
        for phase in range(phases):
            for h, g in order:
                cb_copy(layer, phase, h, g).wait_recv()
                total = cb_send[layer, phase, h, g].astype(jnp.float32) + cb_recv[layer, phase, h, g].astype(jnp.float32)
                if phase < phases - 1:
                    cb_send[layer, phase + 1, h, g] = total.astype(jnp.bfloat16)
                    cb_copy(layer, phase + 1, h, g).start()
                else:
                    lo = h * half + g * rows_of
                    old = (tokens if layer == 0 else stream)[lo:lo + rows_of, :].astype(jnp.float32)
                    new = (RESID * old + total * dscale[...][None, :]).astype(jnp.bfloat16)
                    if layer == 0:
                        stream[lo:lo + rows_of, :] = new
                    else:
                        out[lo:lo + rows_of, :] = new

    for layer in range(2):
        for way, (group, (owner, first, end, sides, _, _)) in itertools.product(range(2), enumerate(groups)):
            at, side, hops, inward, outward = role(way, owner)

            @pl.when(at != owner)
            def _():
                sq_copy(layer, way, group, side, inward).wait_send()

                @pl.loop(first, end)
                def _(k):
                    rs_copy(layer, way, side, k, inward).wait_send()

            @pl.when((at != owner) & (hops > 0))
            def _():
                @pl.loop(first, end)
                def _(k):
                    ag_copy(layer, way, side, k, outward).wait_send()

            @pl.when(at == owner)
            def _():
                @pl.loop(first, end)
                def _(k):
                    for s in sides:
                        ag_copy(layer, way, s, k, outward).wait_send()

        for phase in range(phases):
            for h in range(2):
                for g in range(PIECES):
                    cb_copy(layer, phase, h, g).wait_send()


def solution(mesh):
    n_ra, n_cb = mesh.shape["ra"], mesh.shape["cb"]
    names = ("tokens", "g1", "wg1", "gs1", "wu1", "us1", "wd1", "ds1", "g2", "wg2", "gs2", "wu2", "us2", "wd2", "ds2")

    def body(*args):
        a = dict(zip(names, args))
        small = [a[k] for k in ("g1", "gs1", "us1", "ds1", "g2", "gs2", "us2", "ds2")]
        big = [a[k] for k in ("wg1", "wu1", "wd1", "wg2", "wu2", "wd2")]
        tok, dim = a["tokens"].shape
        ff = a["wg1"].shape[1]
        chunks, half, phases = ff // CHUNK, tok // 2, n_cb.bit_length() - 1
        f32, bf16, dma = jnp.float32, jnp.bfloat16, pltpu.SemaphoreType.DMA
        vmem = pl.BlockSpec(memory_space=pltpu.VMEM)
        piece = (2, phases, 2, PIECES)
        return pl.pallas_call(
            functools.partial(kernel, n_ra, n_cb, dim * n_ra),
            out_shape=jax.ShapeDtypeStruct((tok, dim), bf16),
            in_specs=[pl.BlockSpec(memory_space=pl.ANY)] * 15,
            out_specs=vmem,
            scratch_shapes=[
                pltpu.VMEM((tok, dim), bf16), *[pltpu.VMEM(v.shape, f32) for v in small],
                pltpu.VMEM((2, dim, ff), f32), pltpu.VMEM((2, dim, ff), f32), pltpu.VMEM((2, ff, dim), f32),
                pltpu.VMEM((chunks, tok, 2 * CHUNK), f32),
                pltpu.VMEM((2, 2, chunks, half, 2 * CHUNK), bf16),
                pltpu.VMEM((2, 2, 2, chunks, half, 2 * CHUNK), bf16),
                pltpu.VMEM((2, tok, ff), bf16),
                pltpu.VMEM((2, 2, 2, 8, tok), f32), pltpu.VMEM((2, 2, 2, 2, 8, tok), f32),
                pltpu.VMEM((2, half, 128), f32),
                pltpu.VMEM((tok, dim), bf16), pltpu.VMEM((tok, dim), bf16),
                pltpu.VMEM(piece + (half // PIECES, dim), bf16), pltpu.VMEM(piece + (half // PIECES, dim), bf16),
                dma((9,)), dma((2, chunks)), dma((2, chunks)), dma((2,)),
                dma((2, 2, chunks)), dma((2, 2, 2, chunks)), dma((2, 2, 2, chunks)), dma((2, 2, chunks)),
                dma((2, 2, 2)), dma((2, 2, 2, 2)), dma(piece), dma(piece),
            ],
            compiler_params=pltpu.CompilerParams(
                collective_id=0, has_side_effects=True, vmem_limit_bytes=56 * 1024 * 1024),
        )(a["tokens"], *small, *big)

    in_specs = (
        P("dp", "ra"),
        P("ra"), P("ra", "cb"), P("cb"), P("ra", "cb"), P("cb"), P("cb", "ra"), P("ra"),
        P("ra"), P("ra", "cb"), P("cb"), P("ra", "cb"), P("cb"), P("cb", "ra"), P("ra"),
    )
    return jax.shard_map(body, mesh=mesh, in_specs=in_specs, out_specs=P("dp", "ra"), check_vma=False)
```
